32 devices in a mesh: sp: 16 (over z, y, x), tp: 2 (over core).
Axes of the slice: x: 2, y: 2, z: 4, core: 2. Of those that a mesh axis runs over, the one named last changes fastest.
Arguments:
- hidden_in: bfloat16 [6144, 2048], P('sp'), may hold values from -6 to 6
- drive: bfloat16 [6144, 1024], P('sp', 'tp'), may hold values from -24 to 24
- wide_poles: float32 [2, 32, 64], P(None, 'tp'), may hold values from -2 to 256, as said below
- narrow_poles: float32 [2, 32, 32], P(None, 'tp'), may hold values from -2 to 128, as said below
- log_step: float32 [32, 2], P('tp'), may hold values from -3.912 to -2.526
- forget: float32 [32, 2, 6144], P('tp', None, 'sp'), may hold values from 0 to 2
- wide_input: bfloat16 [2, 32, 64, 16], P(None, 'tp'), may hold values from -1 to 1
- narrow_input: bfloat16 [2, 32, 32, 16], P(None, 'tp'), may hold values from -1 to 1
- wide_output: bfloat16 [2, 32, 16, 64], P(None, 'tp'), may hold values from -0.5 to 0.5
- narrow_output: bfloat16 [2, 32, 16, 32], P(None, 'tp'), may hold values from -0.75 to 0.75
- skip: float32 [1024], P('tp'), may hold values from -4 to 4
- mix_gain: float32 [1024], P('tp'), may hold values from 0.1 to 1.9
- out_weight: bfloat16 [1024, 2048], P('tp'), may hold values from -0.1875 to 0.1875
- mlp_gain: float32 [2048], replicated, may hold values from 0.1 to 1.9
- up_weight: bfloat16 [2048, 8192], P('sp', 'tp'), may hold values from -0.125 to 0.125
- down_weight: bfloat16 [2048, 8192], P('sp', 'tp'), may hold values from -0.0625 to 0.0625
Outputs:
- hidden_out: bfloat16 [6144, 2048], P('sp')
The draws below stay inside these ranges and needn't reach their ends.
Inputs may be any that keep to these rules, and one draw needn't show every extreme that they name: `wide_poles`: entry 0 holds real parts, each at most -1 / 6144; entry 1 holds imaginary parts. `narrow_poles`: entry 0 holds real parts, each at most -1 / 6144; entry 1 holds imaginary parts.
All inputs are finite; a program needn't handle non-finite values.
Results may differ from the reference program's by a relative error of at most 0.02.
Values may be sent and summed in bfloat16 or wider, within the bound.
A program may use at most 128 MiB of HBM per device.

```python
import math
import jax
import jax.numpy as jnp
from jax import lax

D = 2048
FF = 8192
PAIRS = 32
GROUP = 16
SW = 64
SN = 32
TOK_DEV = 384
TOKEN_POSITIONS = 6144
CHANNELS = 1024
N_TP = 2


def pole_draw(key, state_len):
    random_subkeys = jax.random.split(key, 4)
    slow_share = 0.5
    slow_mask = jax.random.uniform(random_subkeys[0], (PAIRS, 1), jnp.float32) < slow_share
    fast_real = -jax.random.uniform(random_subkeys[1], (PAIRS, state_len), jnp.float32, 0.3, 1.6)
    slow_real = -jax.random.uniform(random_subkeys[2], (PAIRS, state_len), jnp.float32, 0.05, 0.15) / (0.05 * TOKEN_POSITIONS)
    real_part = jnp.where(slow_mask, slow_real, fast_real)
    imag_part = math.pi * jnp.arange(state_len, dtype=jnp.float32)[None, :] + jax.random.uniform(random_subkeys[3], (PAIRS, state_len), jnp.float32, -0.5, 0.5)
    return jnp.stack([real_part, imag_part])


def draw_wide_poles(key, part):
    return pole_draw(jax.random.fold_in(key, 11), SW)


def draw_narrow_poles(key, part):
    return pole_draw(jax.random.fold_in(key, 12), SN)


def draw_forget(key, part):
    random_subkeys = jax.random.split(key, 5)
    devices_along = TOKEN_POSITIONS // TOK_DEV
    parity = jax.random.randint(random_subkeys[0], (), 0, 2)
    parity_sign = jnp.where((jnp.arange(devices_along) + parity) % 2 == 0, 1.0, -1.0)
    block_level = jnp.exp(math.log(2.0) * parity_sign * jax.random.uniform(random_subkeys[1], (devices_along,), jnp.float32, 0.5, 1.0))
    per_position = jnp.repeat(block_level, TOK_DEV, total_repeat_length=TOKEN_POSITIONS)
    rough_low = 0.3
    rough_high = 1.7
    level_scale = 1.0
    roughness = jax.random.uniform(random_subkeys[2], (PAIRS, 2, TOKEN_POSITIONS), jnp.float32, rough_low, rough_high)
    baseline_level = level_scale / TOKEN_POSITIONS * per_position[None, None, :] * roughness
    spike_position = jax.random.randint(random_subkeys[3], (3,), 0, TOKEN_POSITIONS)
    spike_amount = jax.random.uniform(random_subkeys[4], (3,), jnp.float32, 0.22, 0.3)
    spike_signal = jnp.sum((jnp.arange(TOKEN_POSITIONS)[None, :] == spike_position[:, None]).astype(jnp.float32) * spike_amount[:, None], axis=0)
    return baseline_level + spike_signal[None, None, :]


def draw_drive(key, part):
    random_subkeys = jax.random.split(key, 3)
    columns = jnp.arange(CHANNELS, dtype=jnp.float32) / CHANNELS
    column_scale = jnp.exp(math.log(0.5) + math.log(6.0) * columns + jax.random.uniform(random_subkeys[0], (CHANNELS,), jnp.float32, -0.35, 0.35))
    row_scale = jnp.exp(jax.random.uniform(random_subkeys[1], (TOKEN_POSITIONS, 1), jnp.float32, math.log(0.3), math.log(3.2)))
    values = jax.random.normal(random_subkeys[2], (TOKEN_POSITIONS, CHANNELS), jnp.float32)
    return jnp.clip(values * row_scale * column_scale[None, :], -24.0, 24.0).astype(jnp.bfloat16)


def level_of(rng, dims, pieces, smallest, high):
    factor_of, own = 1.0, jax.random.fold_in(rng, 6)
    for dim, shards_of in pieces:
        steps = jnp.exp(jax.random.uniform(jax.random.fold_in(own, dim), (shards_of,), jnp.float32, smallest / len(pieces), high / len(pieces)))
        factor_of = factor_of * jnp.repeat(steps, dims[dim] // shards_of).reshape([-1 if axis == dim else 1 for axis in range(len(dims))])
    return factor_of


def normal_values(own_key, shape, width, limit, cuts=(), kind=jnp.bfloat16):
    drawn = jax.random.normal(own_key, shape, jnp.float32) * width
    if len(cuts) > 0:
        drawn = level_of(own_key, shape, cuts, -0.22, 0.18) * drawn
    return jnp.clip(drawn, min=-limit, max=limit).astype(kind)


def setup_inputs(seed: int = 0) -> dict:
    arg_keys = jax.random.split(jax.random.key(seed), 17)
    return {
        "hidden_in": normal_values(arg_keys[0], (TOKEN_POSITIONS, D), 1.0, 6.0, ((0, 16),)),
        "drive": draw_drive(jax.random.fold_in(arg_keys[16], 71), 0),
        "wide_poles": draw_wide_poles(jax.random.fold_in(arg_keys[16], 71), 0),
        "narrow_poles": draw_narrow_poles(jax.random.fold_in(arg_keys[16], 71), 0),
        "log_step": jnp.clip(-3.912 + 1.3859999 * jax.random.uniform(arg_keys[4], (PAIRS, 2), jnp.float32) ** level_of(arg_keys[4], (PAIRS, 2), ((0, 2),), -0.2, 0.2), -3.912, -2.526),
        "forget": draw_forget(jax.random.fold_in(arg_keys[16], 71), 0),
        "wide_input": normal_values(arg_keys[6], (2, PAIRS, SW, GROUP), (2 * GROUP) ** -0.5, 1.0, ((1, 2),)),
        "narrow_input": normal_values(arg_keys[7], (2, PAIRS, SN, GROUP), (2 * GROUP) ** -0.5, 1.0, ((1, 2),)),
        "wide_output": normal_values(arg_keys[8], (2, PAIRS, GROUP, SW), (2 * SW) ** -0.5, 0.5, ((1, 2),)),
        "narrow_output": normal_values(arg_keys[9], (2, PAIRS, GROUP, SN), (2 * SN) ** -0.5, 0.75, ((1, 2),)),
        "skip": normal_values(arg_keys[10], (CHANNELS,), 1.0, 4.0, ((0, 2),), jnp.float32),
        "mix_gain": jnp.clip(1.0 + 0.18 * jax.random.normal(arg_keys[11], (CHANNELS,), jnp.float32), 0.1, 1.9),
        "out_weight": normal_values(arg_keys[12], (CHANNELS, D), CHANNELS ** -0.5, 0.1875, ((0, 2),)),
        "mlp_gain": jnp.clip(1.0 + 0.18 * jax.random.normal(arg_keys[13], (D,), jnp.float32), 0.1, 1.9),
        "up_weight": normal_values(arg_keys[14], (D, FF), D ** -0.5, 0.125, ((0, 16), (1, 2))),
        "down_weight": normal_values(arg_keys[15], (D, FF), FF ** -0.5, 0.0625, ((0, 16), (1, 2))),
    }


epsilon = 1e-06

def combine(earlier, later):
    return (later[0] * earlier[0] - later[1] * earlier[1], later[0] * earlier[1] + later[1] * earlier[0], later[0] * earlier[2] - later[1] * earlier[3] + later[2], later[0] * earlier[3] + later[1] * earlier[2] + later[3])

def discretize(pole_pair, log_rate):
    step_size = jnp.exp(log_rate)[:, None]
    growth = pole_pair[0] * step_size
    angle = pole_pair[1] * step_size
    rise_real = jnp.expm1(growth) * jnp.cos(angle) - 2.0 * jnp.sin(0.5 * angle) ** 2
    rise_imag = jnp.exp(growth) * jnp.sin(angle)
    denominator = pole_pair[0] ** 2 + pole_pair[1] ** 2
    coef_real = (rise_real * pole_pair[0] + rise_imag * pole_pair[1]) / denominator
    coef_imag = (rise_imag * pole_pair[0] - rise_real * pole_pair[1]) / denominator
    return (growth, angle, coef_real, coef_imag)

def kind_states(signal_rows, decay_rows, terms, in_weight):
    growth, angle, coef_real, coef_imag = terms
    drive_real = jnp.einsum('rpg,psg->rps', signal_rows, in_weight[0].astype(jnp.float32))
    drive_imag = jnp.einsum('rpg,psg->rps', signal_rows, in_weight[1].astype(jnp.float32))
    push_real = coef_real * drive_real - coef_imag * drive_imag
    push_imag = coef_real * drive_imag + coef_imag * drive_real
    spike_magnitude = jnp.exp(growth[None] - decay_rows[:, :, None])
    return lax.associative_scan(combine, (spike_magnitude * jnp.cos(angle)[None], spike_magnitude * jnp.sin(angle)[None], push_real, push_imag), axis=0)

def read_out(state_real, state_imag, out_kind):
    first = jnp.einsum('rps,pgs->rpg', state_real, out_kind[0].astype(jnp.float32), precision=lax.Precision.HIGHEST)
    second = jnp.einsum('rps,pgs->rpg', state_imag, out_kind[1].astype(jnp.float32), precision=lax.Precision.HIGHEST)
    return first - second

def row_norm(rows_in, gain):
    values = rows_in.astype(jnp.float32)
    return (values * lax.rsqrt(lax.optimization_barrier(jnp.mean(values * values, axis=1, keepdims=True)) + epsilon) * gain).astype(jnp.bfloat16)

def reference(hidden_in, drive, wide_poles, narrow_poles, log_step, forget, wide_input, narrow_input, wide_output, narrow_output, skip, mix_gain, out_weight, mlp_gain, up_weight, down_weight):
    block_len = math.gcd(TOKEN_POSITIONS, 512)
    block_count = TOKEN_POSITIONS // block_len
    signal = drive.astype(jnp.float32).reshape(block_count, block_len, PAIRS, 2, GROUP)
    decay_all = jnp.transpose(forget, (2, 0, 1)).reshape(block_count, block_len, PAIRS, 2)
    kinds = ((wide_poles, wide_input, wide_output), (narrow_poles, narrow_input, narrow_output))
    responses = []
    for kind_index in range(2):
        pole_pair, in_weight, out_kind = kinds[kind_index]
        terms = discretize(pole_pair, log_step[:, kind_index])

        def advance(carried, block_inputs):
            cum_real, cum_imag, local_real, local_imag = kind_states(block_inputs[0], block_inputs[1], terms, in_weight)
            state_real = local_real + cum_real * carried[0][None] - cum_imag * carried[1][None]
            state_imag = local_imag + cum_real * carried[1][None] + cum_imag * carried[0][None]
            return ((state_real[-1], state_imag[-1]), read_out(state_real, state_imag, out_kind))
        initial = (jnp.zeros(pole_pair.shape[1:], jnp.float32), jnp.zeros(pole_pair.shape[1:], jnp.float32))
        _, block_outputs = lax.scan(advance, initial, (signal[:, :, :, kind_index], decay_all[:, :, :, kind_index]))
        responses.append(block_outputs.reshape(TOKEN_POSITIONS, PAIRS, GROUP))
    response = jnp.stack(responses, axis=2).reshape(TOKEN_POSITIONS, CHANNELS) + skip[None, :] * drive.astype(jnp.float32)
    active = jax.nn.gelu(response, approximate=False)
    mixed = (active * lax.rsqrt(lax.optimization_barrier(jnp.mean(active * active, axis=1, keepdims=True)) + epsilon) * mix_gain).astype(jnp.bfloat16)
    shard_width = CHANNELS // N_TP
    proj_sum = jnp.zeros((TOKEN_POSITIONS, D), jnp.float32)
    for shard_index in range(N_TP):
        low_edge = shard_index * shard_width
        partial_value = jnp.dot(mixed[:, low_edge:low_edge + shard_width], out_weight[low_edge:low_edge + shard_width], preferred_element_type=jnp.float32)
        proj_sum = proj_sum + lax.optimization_barrier(partial_value.astype(jnp.bfloat16)).astype(jnp.float32)
    carried_rows = (hidden_in.astype(jnp.float32) + proj_sum).astype(jnp.bfloat16)
    normed = row_norm(carried_rows, mlp_gain)
    hidden_width = FF // N_TP
    mixer_sum = jnp.zeros((TOKEN_POSITIONS, D), jnp.float32)
    for shard_index in range(N_TP):
        low_edge = shard_index * hidden_width
        pre_act = jnp.dot(normed, up_weight[:, low_edge:low_edge + hidden_width], preferred_element_type=jnp.float32)
        squared = jnp.square(jax.nn.relu(pre_act)).astype(jnp.bfloat16)
        partial_value = lax.dot_general(squared, down_weight[:, low_edge:low_edge + hidden_width], (((1,), (1,)), ((), ())), preferred_element_type=jnp.float32)
        mixer_sum = mixer_sum + lax.optimization_barrier(partial_value.astype(jnp.bfloat16)).astype(jnp.float32)
    return (carried_rows.astype(jnp.float32) + mixer_sum).astype(jnp.bfloat16)
```

```python
import jax
import jax.numpy as jnp
from jax import lax
from jax.experimental import pallas as pl
from jax.experimental.pallas import tpu as pltpu
from jax.sharding import PartitionSpec as P

epsilon = 1e-06
SEGMENTS = 8
HIGHEST = lax.Precision.HIGHEST


def swap(value, axis, shift):
    count = lax.axis_size(axis)
    return lax.ppermute(value, axis, [(i, i ^ shift) for i in range(count)])


def group_of(count):
    return 4 if count % 4 == 0 else (2 if count % 2 == 0 else 1)


def discretize(pole_pair, log_rate):
    step_size = jnp.exp(log_rate)[:, None]
    growth = pole_pair[0] * step_size
    angle = pole_pair[1] * step_size
    rise_real = jnp.expm1(growth) * jnp.cos(angle) - 2.0 * jnp.sin(0.5 * angle) ** 2
    rise_imag = jnp.exp(growth) * jnp.sin(angle)
    denominator = pole_pair[0] ** 2 + pole_pair[1] ** 2
    coef_real = (rise_real * pole_pair[0] + rise_imag * pole_pair[1]) / denominator
    coef_imag = (rise_imag * pole_pair[0] - rise_real * pole_pair[1]) / denominator
    base_real = jnp.exp(growth) * jnp.cos(angle)
    base_imag = jnp.exp(growth) * jnp.sin(angle)
    return jnp.stack([part.reshape(-1) for part in (base_real, base_imag, coef_real, coef_imag)])


def power(real, imag, exponent):
    result = None
    while exponent:
        if exponent & 1:
            result = (
                (real, imag)
                if result is None
                else (result[0] * real - result[1] * imag, result[0] * imag + result[1] * real)
            )
        exponent >>= 1
        if exponent:
            real, imag = (real * real - imag * imag, 2.0 * real * imag)
    return result


def in_matrix(in_weight, kind_index):
    pairs, states, group = in_weight.shape[1:]
    diagonal = jnp.eye(pairs, dtype=jnp.bfloat16)
    select = (jnp.arange(2) == kind_index).astype(jnp.bfloat16)
    return jnp.einsum("pq,k,rpsh->pkhrqs", diagonal, select, in_weight).reshape(
        pairs * 2 * group, 2, pairs * states
    )


def out_matrix(out_kind, kind_index):
    pairs, group, states = out_kind.shape[1:]
    diagonal = jnp.eye(pairs, dtype=jnp.bfloat16)
    select = (jnp.arange(2) == kind_index).astype(jnp.bfloat16)
    signed = out_kind * jnp.array([1, -1], jnp.bfloat16)[:, None, None, None]
    return jnp.einsum("qp,k,rpgs->rqspkg", diagonal, select, signed).reshape(
        2, pairs * states, pairs * 2 * group
    )


def run_scan(decay_ref, pushed_ref, param_ref, start, keep):
    width = decay_ref.shape[1]
    steps = decay_ref.shape[0] // SEGMENTS

    def step(index, state):
        rows = pl.ds(pl.multiple_of(index * SEGMENTS, SEGMENTS), SEGMENTS)
        decay = decay_ref[rows, :]
        real = decay * param_ref[0:1, :]
        imag = decay * param_ref[1:2, :]
        new_real = real * state[0] - imag * state[1] + pushed_ref[rows, :width]
        new_imag = real * state[1] + imag * state[0] + pushed_ref[rows, width:]
        if keep is not None:
            keep[rows, :width] = new_real
            keep[rows, width:] = new_imag
        return (new_real, new_imag)

    return lax.fori_loop(0, steps, step, start)


def ends_kernel(drive_ref, in_ref, decay_ref, total_ref, param_ref, pushed_ref, seg_ref, end_ref):
    width = decay_ref.shape[1]
    pushed = jnp.dot(drive_ref[...], in_ref[...], preferred_element_type=jnp.float32)
    coef_real, coef_imag = param_ref[2:3, :], param_ref[3:4, :]
    pushed_ref[:, :width] = coef_real * pushed[:, :width] - coef_imag * pushed[:, width:]
    pushed_ref[:, width:] = coef_real * pushed[:, width:] + coef_imag * pushed[:, :width]
    zero = jnp.zeros((SEGMENTS, width), jnp.float32)
    real, imag = run_scan(decay_ref, pushed_ref, param_ref, (zero, zero), None)
    seg_ref[:SEGMENTS, :] = real
    seg_ref[SEGMENTS:, :] = imag
    end_real, end_imag = real[0:1], imag[0:1]
    magnitude = total_ref[0:1, :]
    for segment in range(1, SEGMENTS):
        here = total_ref[segment : segment + 1, :]
        across_real, across_imag = here * param_ref[4:5, :], here * param_ref[5:6, :]
        end_real, end_imag = (
            across_real * end_real - across_imag * end_imag + real[segment : segment + 1],
            across_real * end_imag + across_imag * end_real + imag[segment : segment + 1],
        )
        magnitude = magnitude * here
    end_ref[0:1, :] = end_real
    end_ref[1:2, :] = end_imag
    end_ref[2:3, :] = magnitude
    end_ref[3:8, :] = jnp.zeros((5, width), jnp.float32)


def states_kernel(
    pushed_ref, decay_ref, total_ref, param_ref, seg_ref, chain_ref, out_ref, response_ref,
    state_ref, start_ref,
):
    width = decay_ref.shape[1]

    def hop(index, entering):
        row = pl.ds(index, 1)
        real, imag = chain_ref[0, row, :], chain_ref[1, row, :]
        return (
            real * entering[0] - imag * entering[1] + chain_ref[2, row, :],
            real * entering[1] + imag * entering[0] + chain_ref[3, row, :],
        )

    zero = jnp.zeros((1, width), jnp.float32)
    real, imag = lax.fori_loop(0, chain_ref.shape[1], hop, (zero, zero))
    for segment in range(SEGMENTS):
        start_ref[segment : segment + 1, :] = real
        start_ref[SEGMENTS + segment : SEGMENTS + segment + 1, :] = imag
        here = total_ref[segment : segment + 1, :]
        across_real, across_imag = here * param_ref[4:5, :], here * param_ref[5:6, :]
        real, imag = (
            across_real * real - across_imag * imag + seg_ref[segment : segment + 1, :],
            across_real * imag + across_imag * real
            + seg_ref[SEGMENTS + segment : SEGMENTS + segment + 1, :],
        )
    run_scan(
        decay_ref, pushed_ref, param_ref, (start_ref[:SEGMENTS, :], start_ref[SEGMENTS:, :]),
        state_ref,
    )
    states = state_ref[...]
    high = states.astype(jnp.bfloat16)
    low = (states - high.astype(jnp.float32)).astype(jnp.bfloat16)
    response_ref[...] = jnp.dot(
        high, out_ref[...], preferred_element_type=jnp.float32
    ) + jnp.dot(low, out_ref[...], preferred_element_type=jnp.float32)


def state_response(
    drive, poles, log_step, forget, in_weights, out_weights
):
    rows, channels = drive.shape
    steps = rows // SEGMENTS
    param = jnp.concatenate(
        [discretize(poles[kind], log_step[:, kind]) for kind in range(2)], axis=1
    )
    width = param.shape[1]
    over_segment = power(param[0], param[1], steps)
    over_device = power(over_segment[0], over_segment[1], SEGMENTS)
    param = jnp.concatenate([param, jnp.stack(over_segment + over_device)], axis=0)
    in_all = jnp.concatenate(
        [in_matrix(in_weights[kind], kind) for kind in range(2)], axis=2
    ).reshape(channels, 2 * width)
    out_all = jnp.concatenate(
        [out_matrix(out_weights[kind], kind) for kind in range(2)], axis=1
    ).reshape(2 * width, channels)
    pairs = forget.shape[0]
    eye = jnp.eye(pairs, dtype=jnp.float32)
    spread = jnp.concatenate(
        [
            jnp.stack([jnp.repeat(eye, poles[0].shape[2], axis=1), jnp.zeros((pairs, pairs * poles[0].shape[2]), jnp.float32)], axis=1),
            jnp.stack([jnp.zeros((pairs, pairs * poles[1].shape[2]), jnp.float32), jnp.repeat(eye, poles[1].shape[2], axis=1)], axis=1),
        ],
        axis=2,
    ).reshape(2 * pairs, width)
    parted = forget.reshape(2 * pairs, SEGMENTS, steps)
    row_decay = jnp.exp(-parted).transpose(2, 1, 0).reshape(rows, 2 * pairs)
    decay = jnp.dot(row_decay, spread, precision=HIGHEST)
    total = jnp.dot(jnp.exp(-jnp.sum(parted, axis=2)).T, spread, precision=HIGHEST)
    shuffled = drive.reshape(SEGMENTS, steps, channels).transpose(1, 0, 2).reshape(rows, channels)
    f32 = jnp.float32
    flops = 2 * rows * channels * 2 * width
    pushed, segs, ends = pl.pallas_call(
        ends_kernel,
        name="segment_ends",
        out_shape=(
            jax.ShapeDtypeStruct((rows, 2 * width), f32),
            jax.ShapeDtypeStruct((2 * SEGMENTS, width), f32),
            jax.ShapeDtypeStruct((8, width), f32),
        ),
        cost_estimate=pl.CostEstimate(
            flops=flops, bytes_accessed=16 * rows * width, transcendentals=0
        ),
    )(shuffled, in_all, decay, total, param)
    pieces = lax.all_gather(ends[:3], "sp")
    count = pieces.shape[0]
    before = (jnp.arange(count) < lax.axis_index("sp"))[:, None]
    chain = jnp.stack(
        [
            jnp.where(before, pieces[:, 2] * param[6][None], 1.0),
            jnp.where(before, pieces[:, 2] * param[7][None], 0.0),
            jnp.where(before, pieces[:, 0], 0.0),
            jnp.where(before, pieces[:, 1], 0.0),
        ]
    )
    response = pl.pallas_call(
        states_kernel,
        name="states_and_response",
        out_shape=jax.ShapeDtypeStruct((rows, channels), f32),
        scratch_shapes=[
            pltpu.VMEM((rows, 2 * width), f32),
            pltpu.VMEM((2 * SEGMENTS, width), f32),
        ],
        cost_estimate=pl.CostEstimate(
            flops=2 * flops, bytes_accessed=16 * rows * width, transcendentals=0
        ),
    )(pushed, decay, total, param, segs, chain, out_all)
    return response.reshape(steps, SEGMENTS, channels).transpose(1, 0, 2).reshape(rows, channels)


def local(
    hidden_in,
    drive,
    wide_poles,
    narrow_poles,
    log_step,
    forget,
    wide_input,
    narrow_input,
    wide_output,
    narrow_output,
    skip,
    mix_gain,
    out_weight,
    mlp_gain,
    up_weight,
    down_weight,
):
    sp_count, tp_count = lax.axis_size("sp"), lax.axis_size("tp")
    group = group_of(sp_count)
    sp_index, tp_index = lax.axis_index("sp"), lax.axis_index("tp")
    member = sp_index % group
    columns = [
        [index for index in range(first, sp_count, group)] for first in range(group)
    ]

    def own_part(weight):
        depth, hidden = weight.shape
        return weight.reshape(depth, group, hidden // group)

    both = jnp.stack([own_part(up_weight), own_part(down_weight)])

    def part_for(who):
        return lax.dynamic_index_in_dim(both, who, axis=2, keepdims=False)

    arrived = [part_for(member)] + [
        swap(part_for(member ^ shift), "sp", shift) for shift in range(1, group)
    ]
    arrived = jnp.stack(arrived)
    ordered = jnp.stack(
        [
            lax.dynamic_index_in_dim(arrived, member ^ who, axis=0, keepdims=False)
            for who in range(group)
        ],
        axis=1,
    )
    ordered = ordered.reshape(2, -1, ordered.shape[-1])
    up_own = lax.all_gather(ordered[0], "sp", axis=0, tiled=True, axis_index_groups=columns)
    down_own = lax.all_gather(ordered[1], "sp", axis=0, tiled=True, axis_index_groups=columns)

    response = state_response(
        drive,
        (wide_poles, narrow_poles),
        log_step,
        forget,
        (wide_input, narrow_input),
        (wide_output, narrow_output),
    )
    response = response + skip[None, :] * drive.astype(jnp.float32)
    active = jax.nn.gelu(response, approximate=False)

    share = drive.shape[0] // tp_count

    def rows_for(array, who):
        return lax.dynamic_slice_in_dim(array, who * share, share, axis=0)

    own_active = [rows_for(active, tp_index)] + [
        swap(rows_for(active, tp_index ^ shift), "tp", shift) for shift in range(1, tp_count)
    ]
    gains = [mix_gain] + [swap(mix_gain, "tp", shift) for shift in range(1, tp_count)]
    projections = [out_weight] + [swap(out_weight, "tp", shift) for shift in range(1, tp_count)]
    square_sum = sum(jnp.sum(part * part, axis=1, keepdims=True) for part in own_active)
    scale = lax.rsqrt(square_sum / (drive.shape[1] * tp_count) + epsilon)
    proj = sum(
        jnp.dot(
            (part * scale * gain).astype(jnp.bfloat16), matrix, preferred_element_type=jnp.float32
        )
        .astype(jnp.bfloat16)
        .astype(jnp.float32)
        for part, gain, matrix in zip(own_active, gains, projections)
    )
    carried = (rows_for(hidden_in, tp_index).astype(jnp.float32) + proj).astype(jnp.bfloat16)
    values = carried.astype(jnp.float32)
    normed = (
        values
        * lax.rsqrt(jnp.mean(values * values, axis=1, keepdims=True) + epsilon)
        * mlp_gain
    ).astype(jnp.bfloat16)

    ups = [up_own] + [swap(up_own, "tp", shift) for shift in range(1, tp_count)]
    downs = [down_own] + [swap(down_own, "tp", shift) for shift in range(1, tp_count)]
    blocks = [normed] + [swap(normed, "sp", shift) for shift in range(1, group)]

    def hidden_units(block):
        return [
            jnp.square(
                jax.nn.relu(jnp.dot(block, up, preferred_element_type=jnp.float32))
            ).astype(jnp.bfloat16)
            for up in ups
        ]

    squared = [hidden_units(block) for block in blocks]

    def contribution(parts):
        return sum(
            lax.dot_general(
                part, down, (((1,), (1,)), ((), ())), preferred_element_type=jnp.float32
            )
            for part, down in zip(parts, downs)
        )

    ff = contribution(squared[0])
    for shift in range(group - 1, 0, -1):
        back = swap(contribution(squared[shift]).astype(jnp.bfloat16), "sp", shift)
        ff = ff + back.astype(jnp.float32)
    mine = (values + ff).astype(jnp.bfloat16)
    result = jnp.zeros(hidden_in.shape, jnp.bfloat16)
    for shift in range(tp_count):
        piece = mine if shift == 0 else swap(mine, "tp", shift)
        result = lax.dynamic_update_slice_in_dim(
            result, piece, (tp_index ^ shift) * share, axis=0
        )
    return result


def solution(mesh):
    return jax.shard_map(
        local,
        mesh=mesh,
        in_specs=(
            P("sp", None),
            P("sp", "tp"),
            P(None, "tp", None),
            P(None, "tp", None),
            P("tp", None),
            P("tp", None, "sp"),
            P(None, "tp", None, None),
            P(None, "tp", None, None),
            P(None, "tp", None, None),
            P(None, "tp", None, None),
            P("tp"),
            P("tp"),
            P("tp", None),
            P(),
            P("sp", "tp"),
            P("sp", "tp"),
        ),
        out_specs=P("sp", None),
        check_vma=False,
    )
```

```python
import jax
import jax.numpy as jnp
from jax import lax
from jax.experimental import pallas as pl
from jax.experimental.pallas import tpu as pltpu
from jax.sharding import PartitionSpec as P

epsilon = 1e-06
SEGMENTS = 8
HIGHEST = lax.Precision.HIGHEST


def swap(value, axis, shift):
    count = lax.axis_size(axis)
    return lax.ppermute(value, axis, [(i, i ^ shift) for i in range(count)])


def group_of(count):
    return 4 if count % 4 == 0 else (2 if count % 2 == 0 else 1)


def discretize(pole_pair, log_rate):
    step_size = jnp.exp(log_rate)[:, None]
    growth = pole_pair[0] * step_size
    angle = pole_pair[1] * step_size
    rise_real = jnp.expm1(growth) * jnp.cos(angle) - 2.0 * jnp.sin(0.5 * angle) ** 2
    rise_imag = jnp.exp(growth) * jnp.sin(angle)
    denominator = pole_pair[0] ** 2 + pole_pair[1] ** 2
    coef_real = (rise_real * pole_pair[0] + rise_imag * pole_pair[1]) / denominator
    coef_imag = (rise_imag * pole_pair[0] - rise_real * pole_pair[1]) / denominator
    base_real = jnp.exp(growth) * jnp.cos(angle)
    base_imag = jnp.exp(growth) * jnp.sin(angle)
    return jnp.stack([part.reshape(-1) for part in (base_real, base_imag, coef_real, coef_imag)])


def power(real, imag, exponent):
    result = None
    while exponent:
        if exponent & 1:
            result = (
                (real, imag)
                if result is None
                else (result[0] * real - result[1] * imag, result[0] * imag + result[1] * real)
            )
        exponent >>= 1
        if exponent:
            real, imag = (real * real - imag * imag, 2.0 * real * imag)
    return result


def spread_rows(small_ref, owner_ref, target_ref):
    group = small_ref.shape[0]
    small, owner = small_ref[...].astype(jnp.float32), owner_ref[0:1, :]
    for index in range(target_ref.shape[0] // group):
        kept = jnp.where(owner == index, small, 0.0)
        target_ref[index * group : (index + 1) * group, :] = kept.astype(jnp.bfloat16)


def run_scan(decay_ref, pushed_ref, param_ref, start, keep):
    width = decay_ref.shape[1]
    steps = decay_ref.shape[0] // SEGMENTS

    def step(index, state):
        rows = pl.ds(pl.multiple_of(index * SEGMENTS, SEGMENTS), SEGMENTS)
        decay = decay_ref[rows, :]
        real = decay * param_ref[0:1, :]
        imag = decay * param_ref[1:2, :]
        new_real = real * state[0] - imag * state[1] + pushed_ref[rows, :width]
        new_imag = real * state[1] + imag * state[0] + pushed_ref[rows, width:]
        if keep is not None:
            keep[rows, :width] = new_real
            keep[rows, width:] = new_imag
        return (new_real, new_imag)

    return lax.fori_loop(0, steps, step, start)


def ends_kernel(
    drive_ref, small_ref, owner_ref, decay_ref, total_ref, param_ref, pushed_ref, seg_ref, end_ref,
    in_ref,
):
    width = decay_ref.shape[1]
    spread_rows(small_ref, owner_ref, in_ref)
    pushed = jnp.dot(drive_ref[...], in_ref[...], preferred_element_type=jnp.float32)
    coef_real, coef_imag = param_ref[2:3, :], param_ref[3:4, :]
    pushed_ref[:, :width] = coef_real * pushed[:, :width] - coef_imag * pushed[:, width:]
    pushed_ref[:, width:] = coef_real * pushed[:, width:] + coef_imag * pushed[:, :width]
    zero = jnp.zeros((SEGMENTS, width), jnp.float32)
    real, imag = run_scan(decay_ref, pushed_ref, param_ref, (zero, zero), None)
    seg_ref[:SEGMENTS, :] = real
    seg_ref[SEGMENTS:, :] = imag
    end_real, end_imag = real[0:1], imag[0:1]
    magnitude = total_ref[0:1, :]
    for segment in range(1, SEGMENTS):
        here = total_ref[segment : segment + 1, :]
        across_real, across_imag = here * param_ref[4:5, :], here * param_ref[5:6, :]
        end_real, end_imag = (
            across_real * end_real - across_imag * end_imag + real[segment : segment + 1],
            across_real * end_imag + across_imag * end_real + imag[segment : segment + 1],
        )
        magnitude = magnitude * here
    end_ref[0:1, :] = magnitude * param_ref[6:7, :]
    end_ref[1:2, :] = magnitude * param_ref[7:8, :]
    end_ref[2:3, :] = end_real
    end_ref[3:4, :] = end_imag


def states_kernel(
    pushed_ref, decay_ref, total_ref, param_ref, seg_ref, enter_ref, small_ref, owner_ref,
    response_ref, state_ref, start_ref, out_ref,
):
    width = decay_ref.shape[1]
    spread_rows(small_ref, owner_ref, out_ref)

    real, imag = enter_ref[2:3, :], enter_ref[3:4, :]
    for segment in range(SEGMENTS):
        start_ref[segment : segment + 1, :] = real
        start_ref[SEGMENTS + segment : SEGMENTS + segment + 1, :] = imag
        here = total_ref[segment : segment + 1, :]
        across_real, across_imag = here * param_ref[4:5, :], here * param_ref[5:6, :]
        real, imag = (
            across_real * real - across_imag * imag + seg_ref[segment : segment + 1, :],
            across_real * imag + across_imag * real
            + seg_ref[SEGMENTS + segment : SEGMENTS + segment + 1, :],
        )
    run_scan(
        decay_ref, pushed_ref, param_ref, (start_ref[:SEGMENTS, :], start_ref[SEGMENTS:, :]),
        state_ref,
    )
    states = state_ref[...]
    high = states.astype(jnp.bfloat16)
    low = (states - high.astype(jnp.float32)).astype(jnp.bfloat16)
    over_states = (((1,), (1,)), ((), ()))
    response_ref[...] = lax.dot_general(
        high, out_ref[...], over_states, preferred_element_type=jnp.float32
    ) + lax.dot_general(low, out_ref[...], over_states, preferred_element_type=jnp.float32)


def join(earlier, later):
    return jnp.stack(
        [
            later[0] * earlier[0] - later[1] * earlier[1],
            later[0] * earlier[1] + later[1] * earlier[0],
            later[0] * earlier[2] - later[1] * earlier[3] + later[2],
            later[0] * earlier[3] + later[1] * earlier[2] + later[3],
        ]
    )


def entering_state(mine, axis):
    index, shift = lax.axis_index(axis), 1
    block = mine
    before = jnp.zeros_like(mine).at[0].set(1.0)
    while shift < lax.axis_size(axis):
        other = swap(block, axis, shift)
        later = (index // shift) % 2 == 1
        before = jnp.where(later, join(other, before), before)
        block = jnp.where(later, join(other, block), join(block, other))
        shift *= 2
    return before


def state_response(
    drive, poles, log_step, forget, in_weights, out_weights
):
    rows, channels = drive.shape
    steps = rows // SEGMENTS
    param = jnp.concatenate(
        [discretize(poles[kind], log_step[:, kind]) for kind in range(2)], axis=1
    )
    width = param.shape[1]
    over_segment = power(param[0], param[1], steps)
    over_device = power(over_segment[0], over_segment[1], SEGMENTS)
    param = jnp.concatenate([param, jnp.stack(over_segment + over_device)], axis=0)
    group = in_weights[0].shape[3]
    small_in = jnp.concatenate(
        [weight.transpose(3, 0, 1, 2).reshape(group, 2, -1) for weight in in_weights], axis=2
    ).reshape(group, 2 * width)
    small_out = jnp.concatenate(
        [weight.transpose(2, 0, 1, 3).reshape(group, 2, -1) for weight in out_weights], axis=2
    )
    small_out = jnp.concatenate([small_out[:, 0], -small_out[:, 1]], axis=1)
    owner = jnp.concatenate(
        [
            2 * (jnp.arange(poles[kind][0].size, dtype=jnp.int32) // poles[kind].shape[2]) + kind
            for kind in range(2)
        ]
    )
    owner = jnp.tile(owner, 2)[None]
    pairs = forget.shape[0]
    eye = jnp.eye(pairs, dtype=jnp.float32)
    spread = jnp.concatenate(
        [
            jnp.stack([jnp.repeat(eye, poles[0].shape[2], axis=1), jnp.zeros((pairs, pairs * poles[0].shape[2]), jnp.float32)], axis=1),
            jnp.stack([jnp.zeros((pairs, pairs * poles[1].shape[2]), jnp.float32), jnp.repeat(eye, poles[1].shape[2], axis=1)], axis=1),
        ],
        axis=2,
    ).reshape(2 * pairs, width)
    parted = forget.reshape(2 * pairs, SEGMENTS, steps)
    row_decay = jnp.exp(-parted).transpose(2, 1, 0).reshape(rows, 2 * pairs)
    decay = jnp.dot(row_decay, spread, precision=HIGHEST)
    total = jnp.dot(jnp.exp(-jnp.sum(parted, axis=2)).T, spread, precision=HIGHEST)
    shuffled = drive.reshape(SEGMENTS, steps, channels).transpose(1, 0, 2).reshape(rows, channels)
    f32 = jnp.float32
    flops = 2 * rows * channels * 2 * width
    pushed, segs, ends = pl.pallas_call(
        ends_kernel,
        name="segment_ends",
        out_shape=(
            jax.ShapeDtypeStruct((rows, 2 * width), f32),
            jax.ShapeDtypeStruct((2 * SEGMENTS, width), f32),
            jax.ShapeDtypeStruct((4, width), f32),
        ),
        scratch_shapes=[pltpu.VMEM((channels, 2 * width), jnp.bfloat16)],
        cost_estimate=pl.CostEstimate(
            flops=flops, bytes_accessed=16 * rows * width, transcendentals=0
        ),
    )(shuffled, small_in, owner, decay, total, param)
    entering = entering_state(ends, "sp")
    response = pl.pallas_call(
        states_kernel,
        name="states_and_response",
        out_shape=jax.ShapeDtypeStruct((rows, channels), f32),
        scratch_shapes=[
            pltpu.VMEM((rows, 2 * width), f32),
            pltpu.VMEM((2 * SEGMENTS, width), f32),
            pltpu.VMEM((channels, 2 * width), jnp.bfloat16),
        ],
        cost_estimate=pl.CostEstimate(
            flops=2 * flops, bytes_accessed=16 * rows * width, transcendentals=0
        ),
    )(pushed, decay, total, param, segs, entering, small_out, owner)
    return response.reshape(steps, SEGMENTS, channels).transpose(1, 0, 2).reshape(rows, channels)


def local(
    hidden_in,
    drive,
    wide_poles,
    narrow_poles,
    log_step,
    forget,
    wide_input,
    narrow_input,
    wide_output,
    narrow_output,
    skip,
    mix_gain,
    out_weight,
    mlp_gain,
    up_weight,
    down_weight,
):
    sp_count, tp_count = lax.axis_size("sp"), lax.axis_size("tp")
    group = group_of(sp_count)
    sp_index, tp_index = lax.axis_index("sp"), lax.axis_index("tp")
    member = sp_index % group
    columns = [
        [index for index in range(first, sp_count, group)] for first in range(group)
    ]

    def own_part(weight):
        size = weight.shape[1] // group

        def part_for(who):
            return lax.dynamic_slice_in_dim(weight, who * size, size, axis=1)

        arrived = jnp.stack(
            [part_for(member)]
            + [swap(part_for(member ^ shift), "sp", shift) for shift in range(1, group)]
        )
        ordered = jnp.concatenate(
            [
                lax.dynamic_index_in_dim(arrived, member ^ who, axis=0, keepdims=False)
                for who in range(group)
            ]
        )
        return lax.all_gather(ordered, "sp", axis=0, tiled=True, axis_index_groups=columns)

    up_own, down_own = own_part(up_weight), own_part(down_weight)

    response = state_response(
        drive,
        (wide_poles, narrow_poles),
        log_step,
        forget,
        (wide_input, narrow_input),
        (wide_output, narrow_output),
    )
    response = response + skip[None, :] * drive.astype(jnp.float32)
    active = jax.nn.gelu(response, approximate=False)

    share = drive.shape[0] // tp_count

    def rows_for(array, who):
        return lax.dynamic_slice_in_dim(array, who * share, share, axis=0)

    own_active = [rows_for(active, tp_index)] + [
        swap(rows_for(active, tp_index ^ shift), "tp", shift) for shift in range(1, tp_count)
    ]
    gains = [mix_gain] + [swap(mix_gain, "tp", shift) for shift in range(1, tp_count)]
    projections = [out_weight] + [swap(out_weight, "tp", shift) for shift in range(1, tp_count)]
    square_sum = sum(jnp.sum(part * part, axis=1, keepdims=True) for part in own_active)
    scale = lax.rsqrt(square_sum / (drive.shape[1] * tp_count) + epsilon)
    proj = sum(
        jnp.dot(
            (part * scale * gain).astype(jnp.bfloat16), matrix, preferred_element_type=jnp.float32
        )
        .astype(jnp.bfloat16)
        .astype(jnp.float32)
        for part, gain, matrix in zip(own_active, gains, projections)
    )
    carried = (rows_for(hidden_in, tp_index).astype(jnp.float32) + proj).astype(jnp.bfloat16)
    values = carried.astype(jnp.float32)
    normed = (
        values
        * lax.rsqrt(jnp.mean(values * values, axis=1, keepdims=True) + epsilon)
        * mlp_gain
    ).astype(jnp.bfloat16)

    ups = [up_own] + [swap(up_own, "tp", shift) for shift in range(1, tp_count)]
    downs = [down_own] + [swap(down_own, "tp", shift) for shift in range(1, tp_count)]
    order = list(range(group - 1, -1, -1))
    block = jnp.concatenate([swap(normed, "sp", shift) if shift else normed for shift in order])
    squared = [
        jnp.square(jax.nn.relu(jnp.dot(block, up, preferred_element_type=jnp.float32))).astype(
            jnp.bfloat16
        )
        for up in ups
    ]
    ff = jnp.zeros((share, normed.shape[1]), jnp.float32)
    at_once = max(group // 2, 1)
    for first in range(0, group, at_once):
        rows = slice(first * share, (first + at_once) * share)
        partial = sum(
            lax.dot_general(
                part[rows], down, (((1,), (1,)), ((), ())), preferred_element_type=jnp.float32
            )
            for part, down in zip(squared, downs)
        ).astype(jnp.bfloat16)
        for place, shift in enumerate(order[first : first + at_once]):
            piece = partial[place * share : (place + 1) * share]
            ff = ff + (swap(piece, "sp", shift) if shift else piece).astype(jnp.float32)
    result, shift = (values + ff).astype(jnp.bfloat16), 1
    while shift < tp_count:
        other = swap(result, "tp", shift)
        later = (tp_index // shift) % 2 == 1
        result = jnp.where(
            later, jnp.concatenate([other, result]), jnp.concatenate([result, other])
        )
        shift *= 2
    return result


def solution(mesh):
    return jax.shard_map(
        local,
        mesh=mesh,
        in_specs=(
            P("sp", None),
            P("sp", "tp"),
            P(None, "tp", None),
            P(None, "tp", None),
            P("tp", None),
            P("tp", None, "sp"),
            P(None, "tp", None, None),
            P(None, "tp", None, None),
            P(None, "tp", None, None),
            P(None, "tp", None, None),
            P("tp"),
            P("tp"),
            P("tp", None),
            P(),
            P("sp", "tp"),
            P("sp", "tp"),
        ),
        out_specs=P("sp", None),
        check_vma=False,
    )
```
